32 devices in a mesh: fs: 8 (over z, y), tp: 4 (over x, core).
Axes of the slice: x: 2, y: 2, z: 4, core: 2. Of those that a mesh axis runs over, the one named last changes fastest.
Arguments:
- inputs: bfloat16 [16384, 2048], P('fs'), may hold values from -6 to 6
- attn_out: bfloat16 [16384, 1024], P('fs', 'tp'), may hold values from -6 to 6
- grad_query: bfloat16 [16384, 1024], P('fs', 'tp'), may hold values from -0.125 to 0.125
- grad_key: bfloat16 [16384, 1024], P('fs', 'tp'), may hold values from -0.125 to 0.125
- grad_mixed: bfloat16 [16384, 2048], P('fs'), may hold values from -0.15625 to 0.15625
- query_weight: float32 [2048, 1024], P('fs', 'tp'), may hold values from -0.75 to 0.75
- key_weight: float32 [2048, 1024], P('fs', 'tp'), may hold values from -0.75 to 0.75
- out_weight: float32 [1024, 2048], P('tp', 'fs'), may hold values from -0.75 to 0.75
- factors: bfloat16 [3, 2048, 256], P(None, 'fs'), may hold values from -0.125 to 0.125
- moment_first: float32 [3, 256, 1024], P(None, 'fs', 'tp'), may hold values from -6 to 6
- moment_second: float32 [3, 256, 1024], P(None, 'fs', 'tp'), may hold values from 0.05 to 2
Outputs:
- step_query: float32 [2048, 1024], P('fs', 'tp')
- step_key: float32 [2048, 1024], P('fs', 'tp')
- step_out: float32 [1024, 2048], P('tp', 'fs')
- copy_query: bfloat16 [2048, 1024], P(None, 'tp')
- copy_key: bfloat16 [2048, 1024], P(None, 'tp')
- copy_out: bfloat16 [1024, 2048], P('tp')
- first_new: float32 [3, 256, 1024], P(None, 'fs', 'tp')
- second_new: float32 [3, 256, 1024], P(None, 'fs', 'tp')
The draws below stay inside these ranges and needn't reach their ends.
All inputs are finite; a program needn't handle non-finite values.
Results may differ from the reference program's by a relative error of at most 0.006.
Values may be sent and summed in bfloat16 or wider, within the bound.
A program may use at most 128 MiB of HBM per device.

```python
import math
import jax
import jax.numpy as jnp
from jax import lax

D = 2048
RANK = 256
TOKENS = 16384
HW = 1024


def spiked(values, key, source, target, blocks, factor):
    owner, partner = [(jnp.arange(values.shape[dim]) // (values.shape[dim] // blocks)).reshape([-1 if axis == dim else 1 for axis in range(values.ndim)]) for dim in (source, target)]
    chosen = jax.random.permutation(key, blocks)[partner]
    strong = (owner == chosen) | (owner == (partner + blocks // 2) % blocks)
    return jnp.where(strong, factor * values, values)


def levels(rng, dims, split, smallest, top_value):
    level, own = 1.0, jax.random.fold_in(rng, 6)
    for position, blocks in split:
        draws = jnp.exp(jax.random.uniform(jax.random.fold_in(own, position), (blocks,), jnp.float32, smallest / len(split), top_value / len(split)))
        level = level * jnp.repeat(draws, dims[position] // blocks).reshape([-1 if axis == position else 1 for axis in range(len(dims))])
    return level


def centred(rng, shape, spread, most, shards=(), held_as=jnp.bfloat16):
    entries = jax.random.normal(rng, shape, jnp.float32) * spread
    if len(shards) > 0:
        entries = levels(rng, shape, shards, -0.22, 0.18) * entries
    return jnp.clip(entries, min=-most, max=most).astype(held_as)


def noise_with(own_key, extent, scale, bound, shards, heavy, dtype=jnp.bfloat16):
    result = scale * jax.random.normal(own_key, extent, jnp.float32)
    if shards:
        result = result * levels(own_key, extent, shards, -0.22, 0.18)
    return jnp.clip(spiked(result, jax.random.fold_in(own_key, 3), *heavy), -bound, bound).astype(dtype)


def setup_inputs(seed: int = 0) -> dict:
    key_of = jax.random.split(jax.random.key(seed), 12)
    inputs = noise_with(key_of[0], (TOKENS, D), 1.0, 6.0, ((0, 8),), (0, 1, 8, 2.0))
    attn_out = centred(key_of[1], (TOKENS, HW), 1.0, 6.0, ((0, 8), (1, 4)))
    grad_query = centred(key_of[2], (TOKENS, HW), (1.0 / TOKENS ** 0.5), 0.125, ((0, 8), (1, 4)))
    grad_key = centred(key_of[3], (TOKENS, HW), (1.0 / TOKENS ** 0.5), 0.125, ((0, 8), (1, 4)))
    grad_mixed = noise_with(key_of[4], (TOKENS, D), (1.0 / TOKENS ** 0.5), 0.15625, ((0, 8),), (0, 1, 8, 2.0))
    query_weight = centred(key_of[5], (D, HW), 0.05, 0.75, ((0, 8), (1, 4)), jnp.float32)
    key_weight = centred(key_of[6], (D, HW), 0.05, 0.75, ((0, 8), (1, 4)), jnp.float32)
    out_weight = centred(key_of[7], (HW, D), 0.05, 0.75, ((0, 4), (1, 8)), jnp.float32)
    factors = centred(key_of[8], (3, D, RANK), D ** -0.5, 0.125, ((1, 8),))
    moment_first = noise_with(key_of[9], (3, RANK, HW), 1.0, 6.0, ((1, 8), (2, 4)), (1, 2, 8, 2.0), jnp.float32)
    moment_second = jnp.clip(jnp.exp(math.log(2.0) - 3.6888794 * jax.random.uniform(key_of[10], (3, RANK, HW), jnp.float32) ** levels(key_of[10], (3, RANK, HW), ((1, 8), (2, 4)), -0.2, 0.2)), 0.05, 2.0)
    return {"inputs": inputs, "attn_out": attn_out, "grad_query": grad_query, "grad_key": grad_key, "grad_mixed": grad_mixed, "query_weight": query_weight, "key_weight": key_weight, "out_weight": out_weight, "factors": factors, "moment_first": moment_first, "moment_second": moment_second}


first_decay = 0.8
second_decay = 0.9
epsilon = 1e-08
learn_rate = 0.02

def project(left_side, right_side, factor_rows):
    mapped = jnp.dot(left_side.astype(jnp.float32), factor_rows.astype(jnp.float32), precision=lax.Precision.HIGHEST)
    return jnp.dot(mapped.T, right_side.astype(jnp.float32), precision=lax.Precision.HIGHEST)

def widen_product(left_side, right_side):
    return jnp.dot(left_side.astype(jnp.float32), right_side.astype(jnp.float32), precision=lax.Precision.HIGHEST)

def reference(inputs, attn_out, grad_query, grad_key, grad_mixed, query_weight, key_weight, out_weight, factors, moment_first, moment_second):
    projected = jnp.stack([project(inputs, grad_query, factors[0]), project(inputs, grad_key, factors[1]), project(grad_mixed, attn_out, factors[2])])
    first_new = first_decay * moment_first + (1.0 - first_decay) * projected
    second_new = second_decay * moment_second + (1.0 - second_decay) * projected * projected
    ratio = first_new / (jnp.sqrt(second_new) + epsilon)
    square_total = jnp.sum(ratio * ratio)
    step_scale = lax.rsqrt(square_total / (3 * RANK * HW) + 1.0)
    ratio_b = ratio.astype(jnp.bfloat16)
    step_query = step_scale * widen_product(factors[0], ratio_b[0])
    step_key = step_scale * widen_product(factors[1], ratio_b[1])
    step_out = step_scale * widen_product(factors[2], ratio_b[2]).T
    copy_query = (query_weight - learn_rate * step_query).astype(jnp.bfloat16)
    copy_key = (key_weight - learn_rate * step_key).astype(jnp.bfloat16)
    copy_out = (out_weight - learn_rate * step_out).astype(jnp.bfloat16)
    return (step_query, step_key, step_out, copy_query, copy_key, copy_out, first_new, second_new)
```

```python
import functools

import jax
import jax.numpy as jnp
from jax import lax
from jax.experimental import pallas as pl
from jax.experimental.pallas import tpu as pltpu
from jax.sharding import PartitionSpec as P

MESH = pl.DeviceIdType.MESH
BF, F32 = jnp.bfloat16, jnp.float32

first_decay = 0.8
second_decay = 0.9
epsilon = 1e-08
learn_rate = 0.02
CHUNKS = 4


def flip(index, bit):
    return index + bit * (1 - 2 * ((index // bit) % 2))


def kernel(
    n, ntp,
    x_hbm, mixed_hbm, gq_ref, gk_ref, ao_ref, wq_ref, wk_ref, wo_ref, f_ref, m1_ref, m2_ref,
    fall_out, wall, r_out, scale_out, first_ref, second_ref,
    xv, gt, fall, wsrc, ps, pr, rsrc, rall, part, parts_tp, psum_fs, parts_fs,
    ld_sem, own_sem, fsend, frecv, wsend, wrecv, psend, precv, rsend, rrecv, ssend, srecv, tsend, trecv,
):
    me, q = lax.axis_index("fs"), lax.axis_index("tp")
    inner, outer = me % 2, me // 2
    nout = n // 2
    rows = f_ref.shape[1]
    rq = rows // ntp
    rk = m1_ref.shape[1]
    depth = x_hbm.shape[1]
    width = depth // CHUNKS
    bits = []
    b = ntp // 2
    while b >= 1:
        bits.append(b)
        b //= 2

    loads = []
    for a, src in enumerate((x_hbm, mixed_hbm)):
        for c in range(CHUNKS):
            cut = pl.ds(c * width, width)
            copy = pltpu.make_async_copy(src.at[:, cut], xv.at[a, :, cut], ld_sem.at[a * CHUNKS + c])
            copy.start()
            loads.append(copy)

    z_peers = [((outer + k) % nout) * 2 + inner for k in range(1, nout)]
    y_peer = me + 1 - 2 * inner
    y_side = [((outer + k) % nout) * 2 + 1 - inner for k in range(1, nout)]
    others = z_peers + [y_peer] + y_side
    tp_peers = [(q + k) % ntp for k in range(1, ntp)]

    barrier = pltpu.get_barrier_semaphore()
    for p in others:
        pl.semaphore_signal(barrier, inc=1, device_id=(p, q), device_id_type=MESH)
    for t in tp_peers:
        pl.semaphore_signal(barrier, inc=1, device_id=(me, t), device_id_type=MESH)
    pl.semaphore_wait(barrier, len(others) + len(tp_peers))

    def remote(src, dst, send, recv, device):
        return pltpu.make_async_remote_copy(
            src_ref=src, dst_ref=dst, send_sem=send, recv_sem=recv, device_id=device, device_id_type=MESH
        )

    def f_piece(ref, p, t):
        return ref.at[:, pl.ds(pl.multiple_of(p * rows + t * rq, rq), rq), :]

    def f_send(p, t, device, own=False):
        src = f_ref.at[:, pl.ds(pl.multiple_of(t * rq, rq), rq), :] if own else f_piece(fall, p, t)
        remote(src, f_piece(fall, p, t), fsend, frecv.at[p, t], device).start()

    def f_wait(p, t):
        remote(f_piece(fall, p, t), f_piece(fall, p, t), fsend, frecv.at[p, t], (me, q)).wait_recv()

    def w_piece(m, p):
        return wall.at[m, pl.ds(pl.multiple_of(p * rows, rows), rows), :]

    def w_own(m, p):
        remote(wsrc.at[m], w_piece(m, me), wsend, wrecv.at[m, me], (p, q)).start()

    def w_wait(m, p):
        remote(w_piece(m, p), w_piece(m, p), wsend, wrecv.at[m, p], (me, q)).wait_recv()

    def w_forward(m, p):
        w_wait(m, p)
        remote(w_piece(m, p), w_piece(m, p), wsend, wrecv.at[m, p], (y_peer, q)).start()

    for p in z_peers:
        f_send(me, q, (p, q), own=True)
    f_send(me, q, (y_peer, q), own=True)

    wsrc[0] = wq_ref[...].astype(BF)
    wsrc[1] = wk_ref[...].astype(BF)
    wsrc[2] = wo_ref[...].T.astype(BF)
    for p in z_peers:
        w_own(0, p)
    keeps = []
    for m in range(3):
        keep = pltpu.make_async_copy(wsrc.at[m], w_piece(m, me), own_sem.at[m])
        keep.start()
        keeps.append(keep)
    fall[:, pl.ds(pl.multiple_of(me * rows, rows), rows), :] = f_ref[...]

    def share(p, t, stage):
        for bit in bits[stage:]:
            f_send(p, t, (me, flip(q, bit)))

    def from_z(p):
        f_wait(p, q)
        f_send(p, q, (y_peer, q))
        share(p, q, 0)

    def from_y(p):
        f_wait(p, q)
        share(p, q, 0)

    tasks = [functools.partial(from_z, p) for p in z_peers]
    tasks.append(functools.partial(from_y, y_peer))
    work = []
    for m in range(3):
        for c in range(CHUNKS):
            work.append((m, c))
    per_task = max(1, -(-len(tasks) // 6))
    lhs = [gq_ref, gk_ref, ao_ref]
    left = None
    for step, (m, c) in enumerate(work):
        if c == 0:
            left = lhs[m][...].T
        a = 0 if m < 2 else 1
        if m != 1:
            loads[a * CHUNKS + c].wait()
        cut = slice(c * width, (c + 1) * width)
        gt[m, :, cut] = jnp.dot(left, xv[a, :, cut], preferred_element_type=F32).astype(BF)
        if step >= 5:
            for task in tasks[:per_task]:
                task()
            tasks = tasks[per_task:]
    for task in tasks:
        task()
    for m in range(3):
        w_own(m, y_peer)
    for p in z_peers:
        w_own(1, p)
    for p in y_side:
        from_y(p)
    held = [q]
    for stage, bit in enumerate(bits):
        arriving = [flip(t, bit) for t in held]
        for p in others:
            for t in arriving:
                f_wait(p, t)
                share(p, t, stage + 1)
        held = held + arriving
    keep_f = pltpu.make_async_copy(fall, fall_out, own_sem.at[3])
    keep_f.start()

    for m in range(3):
        projected = jnp.dot(gt[m], fall[m], preferred_element_type=F32).T
        ps[:, m] = projected.reshape(n, rk, projected.shape[1]).astype(BF)
    for p in others:
        remote(ps.at[p], pr.at[me], psend, precv.at[me], (p, q)).start()
    pr[me] = ps[me]
    for p in z_peers:
        w_own(2, p)
    for p in z_peers:
        w_forward(0, p)
    for p in others:
        remote(pr.at[p], pr.at[p], psend, precv.at[p], (me, q)).wait_recv()
    reduced = pr[0].astype(F32)
    for i in range(1, n):
        reduced = reduced + pr[i].astype(F32)
    first_new = first_decay * m1_ref[...] + (1.0 - first_decay) * reduced
    second_new = second_decay * m2_ref[...] + (1.0 - second_decay) * reduced * reduced
    ratio = first_new / (jnp.sqrt(second_new) + epsilon)
    rsrc[...] = ratio.astype(BF)
    part[...] = jnp.broadcast_to(jnp.sum(ratio * ratio).reshape(1, 1), part.shape)
    for p in z_peers + [y_peer]:
        remote(rsrc, rall.at[me], rsend, rrecv.at[me], (p, q)).start()
    for k, t in enumerate(tp_peers):
        remote(part, parts_tp.at[q], tsend.at[k], trecv.at[q], (me, t)).start()
    first_ref[...] = first_new
    second_ref[...] = second_new
    rall[me] = rsrc[...]
    parts_tp[q] = part[...]
    for t in tp_peers:
        remote(part, parts_tp.at[t], tsend.at[0], trecv.at[t], (me, q)).wait_recv()
    total = parts_tp[0]
    for t in range(1, ntp):
        total = total + parts_tp[t]
    psum_fs[...] = total
    for k, p in enumerate(others):
        remote(psum_fs, parts_fs.at[me], ssend.at[k], srecv.at[me], (p, q)).start()
    parts_fs[me] = total

    def r_wait(p):
        remote(rall.at[p], rall.at[p], rsend, rrecv.at[p], (me, q)).wait_recv()

    for p in z_peers:
        r_wait(p)
        remote(rall.at[p], rall.at[p], rsend, rrecv.at[p], (y_peer, q)).start()
    for m in (1, 2):
        for p in z_peers:
            w_forward(m, p)
    for p in [y_peer] + y_side:
        r_wait(p)
    for m in range(3):
        r_out[m] = rall[:, m].astype(F32).reshape(r_out.shape[1], r_out.shape[2]).astype(BF)
    for p in others:
        remote(psum_fs, parts_fs.at[p], ssend.at[0], srecv.at[p], (me, q)).wait_recv()
    square_total = parts_fs[0]
    for i in range(1, n):
        square_total = square_total + parts_fs[i]
    count = 3 * (rk * n) * (m1_ref.shape[2] * ntp)
    scale_out[...] = lax.rsqrt(square_total / count + 1.0)

    for m in range(3):
        for p in [y_peer] + y_side:
            w_wait(m, p)
    for keep in keeps:
        keep.wait()
    keep_f.wait()
    span = fall.at[:, pl.ds(0, (n - 1) * rows), :]
    remote(span, span, fsend, frecv.at[0, 0], (me, q)).wait_send()
    span = wall.at[:, pl.ds(0, (n - 1) * rows), :]
    remote(span, span, wsend, wrecv.at[0, 0], (me, q)).wait_send()
    span = ps.at[pl.ds(0, n - 1)]
    remote(span, span, psend, precv.at[0], (me, q)).wait_send()
    span = rall.at[pl.ds(0, n - 1)]
    remote(span, span, rsend, rrecv.at[0], (me, q)).wait_send()
    for k, t in enumerate(tp_peers):
        remote(part, part, tsend.at[k], trecv.at[0], (me, q)).wait_send()
    for k, p in enumerate(others):
        remote(psum_fs, psum_fs, ssend.at[k], srecv.at[0], (me, q)).wait_send()


def per_device(
    n, ntp,
    inputs, attn_out, grad_query, grad_key, grad_mixed, query_weight, key_weight, out_weight,
    factors, moment_first, moment_second,
):
    tokens, depth = inputs.shape
    cols = grad_query.shape[1]
    rows, rank = factors.shape[1:]
    rk = moment_first.shape[1]
    anyspace = pl.BlockSpec(memory_space=pl.ANY)
    vmem = pl.BlockSpec(memory_space=pltpu.VMEM)
    dma = pltpu.SemaphoreType.DMA
    shape = jax.ShapeDtypeStruct
    fall, wall, directions, scale, first_new, second_new = pl.pallas_call(
        functools.partial(kernel, n, ntp),
        out_shape=(
            shape((3, depth, rank), BF),
            shape((3, depth, cols), BF),
            shape((3, rank, cols), BF),
            shape((1, 128), F32),
            shape(moment_first.shape, F32),
            shape(moment_second.shape, F32),
        ),
        in_specs=[anyspace] * 2 + [vmem] * 9,
        out_specs=(anyspace, anyspace, vmem, vmem, vmem, vmem),
        scratch_shapes=[
            pltpu.VMEM((2, tokens, depth), BF),
            pltpu.VMEM((3, cols, depth), BF),
            pltpu.VMEM((3, depth, rank), BF),
            pltpu.VMEM((3, rows, cols), BF),
            pltpu.VMEM((n, 3, rk, cols), BF),
            pltpu.VMEM((n, 3, rk, cols), BF),
            pltpu.VMEM((3, rk, cols), BF),
            pltpu.VMEM((n, 3, rk, cols), BF),
            pltpu.VMEM((1, 128), F32),
            pltpu.VMEM((ntp, 1, 128), F32),
            pltpu.VMEM((1, 128), F32),
            pltpu.VMEM((n, 1, 128), F32),
            dma((2 * CHUNKS,)), dma((4,)),
            dma, dma((n, ntp)), dma, dma((3, n)), dma, dma((n,)), dma, dma((n,)),
            dma((n,)), dma((n,)), dma((ntp,)), dma((ntp,)),
        ],
        compiler_params=pltpu.CompilerParams(
            collective_id=0, has_side_effects=True, vmem_limit_bytes=60 * 1024 * 1024
        ),
    )(
        inputs, grad_mixed, grad_query, grad_key, attn_out, query_weight, key_weight, out_weight,
        factors, moment_first, moment_second,
    )
    step_scale = scale[0, 0]

    def product(left, number):
        return jnp.dot(left, directions[number], preferred_element_type=F32)

    step_query = step_scale * product(factors[0], 0)
    step_key = step_scale * product(factors[1], 1)
    step_out = step_scale * product(factors[2], 2).T
    rate = learn_rate * step_scale
    copies = [
        (wall[m].astype(F32) - rate * product(fall[m], m)).astype(BF) for m in range(3)
    ]
    return (step_query, step_key, step_out, copies[0], copies[1], copies[2].T, first_new, second_new)


def solution(mesh):
    in_specs = (
        P("fs", None),
        P("fs", "tp"),
        P("fs", "tp"),
        P("fs", "tp"),
        P("fs", None),
        P("fs", "tp"),
        P("fs", "tp"),
        P("tp", "fs"),
        P(None, "fs", None),
        P(None, "fs", "tp"),
        P(None, "fs", "tp"),
    )
    out_specs = (
        P("fs", "tp"),
        P("fs", "tp"),
        P("tp", "fs"),
        P(None, "tp"),
        P(None, "tp"),
        P("tp", None),
        P(None, "fs", "tp"),
        P(None, "fs", "tp"),
    )
    return jax.shard_map(
        functools.partial(per_device, mesh.shape["fs"], mesh.shape["tp"]),
        mesh=mesh, in_specs=in_specs, out_specs=out_specs, check_vma=False,
    )
```
